32 devices in a mesh: sp: 4 (over y, x), dp: 8 (over z, core).
Axes of the slice: x: 2, y: 2, z: 4, core: 2. Of those that a mesh axis runs over, the one named last changes fastest.
Arguments:
- tokens: bfloat16 [8, 1024, 2048], P('dp', 'sp'), may hold values from -6 to 6
- in_gain: float32 [2048], replicated, may hold values from 0.1 to 1.9
- query_weight: bfloat16 [2048, 2048], P('dp'), may hold values from -1 to 1
- key_weight: bfloat16 [2048, 512], P('dp'), may hold values from -1 to 1
- value_matrix: bfloat16 [2048, 512], P('dp'), may hold values from -0.125 to 0.125
- query_gain: float32 [128], replicated, may hold values from 1 to 6
- key_gain: float32 [128], replicated, may hold values from 1 to 6
- out_weight: bfloat16 [2048, 2048], P('dp'), may hold values from -0.125 to 0.125
- out_gain: float32 [2048], replicated, may hold values from 0.1 to 1.9
Outputs:
- mixed: bfloat16 [8, 1024, 2048], P('dp', 'sp')
The draws below stay inside these ranges and needn't reach their ends.
All inputs are finite; a program needn't handle non-finite values.
Results may differ from the reference program's by a relative error of at most 0.0055.
The reference program's roundings to bfloat16 on the way count: a program that leaves them out, or rounds other values in their place, can miss the bound.
Values may be sent and summed in bfloat16 or wider, within the bound.
A program may use at most 128 MiB of HBM per device.

```python
import jax
import jax.numpy as jnp
from jax import lax

MODEL_WIDTH = 2048
QUERY_HEAD_COUNT = 16
KEY_VALUE_HEADS = 4
HEAD_WIDTH = 128
GRID_W = 64
SEQUENCE_LENGTH = 1024
BATCH = 8


def query_for_group(key):
    return jax.random.truncated_normal(jax.random.fold_in(key, 101), -6.0, 6.0, (MODEL_WIDTH, QUERY_HEAD_COUNT * HEAD_WIDTH), jnp.float32) * MODEL_WIDTH ** (-0.5)


def draw_query_weight(key, part):
    return query_for_group(key).astype(jnp.bfloat16)


def draw_key_weight(key, part):
    complete_output = jax.random.truncated_normal(jax.random.fold_in(key, 401), -6.0, 6.0, (MODEL_WIDTH, KEY_VALUE_HEADS * HEAD_WIDTH), jnp.float32) * MODEL_WIDTH ** (-0.5)
    return complete_output.astype(jnp.bfloat16)


def draw_query_gain(key, part):
    return 1.6 * (1.0 + 0.18 * jax.random.uniform(jax.random.fold_in(key, 201), (HEAD_WIDTH,), jnp.float32, -1.0, 1.0))


def draw_key_gain(key, part):
    return 1.6 * (1.0 + 0.18 * jax.random.uniform(jax.random.fold_in(key, 301), (HEAD_WIDTH,), jnp.float32, -1.0, 1.0))


def level_of(key, dims, split, low, largest):
    def one(dim, shards_of):
        heights = jax.random.uniform(jax.random.fold_in(jax.random.fold_in(key, 6), dim), (shards_of,), jnp.float32, low / len(split), largest / len(split))
        return jnp.repeat(jnp.exp(heights), dims[dim] // shards_of).reshape((-1,) + (1,) * (len(dims) - dim - 1))

    level = one(*split[0])
    for cut in split[1:]:
        level = level * one(*cut)
    return level


def gaussian(rng, extent, deviation, reach, pieces=(), kind=jnp.bfloat16):
    drawn = deviation * jax.random.normal(rng, extent, jnp.float32)
    if pieces:
        drawn = drawn * level_of(rng, extent, pieces, -0.22, 0.18)
    return jnp.clip(drawn, -reach, reach).astype(kind)


def setup_inputs(seed: int = 0) -> dict:
    seeds = jax.random.split(jax.random.key(seed), 10)
    return {
        "tokens": gaussian(seeds[0], (BATCH, SEQUENCE_LENGTH, MODEL_WIDTH), 1.0, 6.0, ((0, 8), (1, 4))),
        "in_gain": jnp.clip(1.0 + 0.18 * jax.random.normal(seeds[1], (MODEL_WIDTH,), jnp.float32), 0.1, 1.9),
        "query_weight": draw_query_weight(jax.random.fold_in(seeds[9], 71), 0),
        "key_weight": draw_key_weight(jax.random.fold_in(seeds[9], 71), 0),
        "value_matrix": gaussian(seeds[4], (MODEL_WIDTH, KEY_VALUE_HEADS * HEAD_WIDTH), MODEL_WIDTH ** -0.5, 0.125, ((0, 8),)),
        "query_gain": draw_query_gain(jax.random.fold_in(seeds[9], 71), 0),
        "key_gain": draw_key_gain(jax.random.fold_in(seeds[9], 71), 0),
        "out_weight": gaussian(seeds[7], (QUERY_HEAD_COUNT * HEAD_WIDTH, MODEL_WIDTH), (QUERY_HEAD_COUNT * HEAD_WIDTH) ** -0.5, 0.125, ((0, 8),)),
        "out_gain": jnp.clip(1.0 + 0.18 * jax.random.normal(seeds[8], (MODEL_WIDTH,), jnp.float32), 0.1, 1.9),
    }


EPS = 1e-06
THETA = 10000.0

def norm_rows(row_data, gain_vec):
    return row_data * lax.rsqrt(lax.optimization_barrier(jnp.mean(row_data * row_data, axis=-1, keepdims=True)) + EPS) * gain_vec.astype(jnp.float32)

def rotate(head_data, positions):
    head_size = head_data.shape[-1]
    half_size = head_size // 2
    quarter = head_size // 4
    inverse_freq = THETA ** (-jnp.arange(quarter, dtype=jnp.float32) / quarter)
    row_angle = (positions // GRID_W).astype(jnp.float32)[:, None] * inverse_freq[None, :]
    col_angle = (positions % GRID_W).astype(jnp.float32)[:, None] * inverse_freq[None, :]

    def turn_half(half_part, angle):
        cosine = jnp.cos(angle)[:, None, :]
        sine_val = jnp.sin(angle)[:, None, :]
        first_part = half_part[..., :quarter]
        second_part = half_part[..., quarter:]
        return jnp.concatenate([first_part * cosine - second_part * sine_val, second_part * cosine + first_part * sine_val], axis=-1)
    return jnp.concatenate([turn_half(head_data[..., :half_size], row_angle), turn_half(head_data[..., half_size:], col_angle)], axis=-1)

def finish(projected, gain_vec, positions):
    row_count = projected.shape[0]
    heads_data = projected.reshape(row_count, -1, HEAD_WIDTH)
    heads_data = rotate(norm_rows(heads_data, gain_vec), positions)
    return heads_data.reshape(row_count, -1).astype(jnp.bfloat16)

def reference(tokens, in_gain, query_weight, key_weight, value_matrix, query_gain, key_gain, out_weight, out_gain):
    queries_per_group = QUERY_HEAD_COUNT // KEY_VALUE_HEADS
    rows_per_block = min(512, SEQUENCE_LENGTH)

    def per_sequence(sequence):
        float_rows = sequence.astype(jnp.float32)
        normed = norm_rows(float_rows, in_gain).astype(jnp.bfloat16)
        positions = jnp.arange(SEQUENCE_LENGTH, dtype=jnp.int32)
        query_rows = finish(jnp.dot(normed, query_weight, preferred_element_type=jnp.float32), query_gain, positions)
        key_matrix_rows = finish(jnp.dot(normed, key_weight, preferred_element_type=jnp.float32), key_gain, positions)
        value_rows = jnp.dot(normed, value_matrix, preferred_element_type=jnp.float32).astype(jnp.bfloat16)
        key_rows_float = key_matrix_rows.reshape(SEQUENCE_LENGTH, KEY_VALUE_HEADS, HEAD_WIDTH).astype(jnp.float32)
        value_rows_float = value_rows.reshape(SEQUENCE_LENGTH, KEY_VALUE_HEADS, HEAD_WIDTH).astype(jnp.float32)
        query_block_list = query_rows.reshape(SEQUENCE_LENGTH // rows_per_block, rows_per_block, KEY_VALUE_HEADS, queries_per_group, HEAD_WIDTH)

        def attend(query_block):
            scores = jnp.einsum('qegd,ked->egqk', query_block.astype(jnp.float32), key_rows_float) * HEAD_WIDTH ** (-0.5)
            shifted = scores - lax.optimization_barrier(jnp.max(scores, axis=-1, keepdims=True))
            raised = jnp.exp(shifted)
            weights = (raised / lax.optimization_barrier(jnp.sum(raised, axis=-1, keepdims=True))).astype(jnp.bfloat16)
            attended = jnp.einsum('egqk,ked->qegd', weights.astype(jnp.float32), value_rows_float)
            return attended.astype(jnp.bfloat16)
        attended = lax.map(attend, query_block_list).reshape(SEQUENCE_LENGTH, QUERY_HEAD_COUNT * HEAD_WIDTH)
        projected = jnp.dot(attended, out_weight, preferred_element_type=jnp.float32)
        return norm_rows(projected, out_gain).astype(jnp.bfloat16)
    return lax.map(per_sequence, tokens)
```

```python
import functools

import jax
import jax.numpy as jnp
import numpy as np
from jax import lax
from jax.experimental import pallas as pl
from jax.experimental.pallas import tpu as pltpu
from jax.sharding import PartitionSpec as P

QUERY_HEAD_COUNT = 16
KEY_VALUE_HEADS = 4
HEAD_WIDTH = 128
GRID_W = 64
EPS = 1e-06
THETA = 10000.0
MESH = pl.DeviceIdType.MESH
ANY = pl.BlockSpec(memory_space=pl.ANY)


def remote(src, dst, send_sem, recv_sem, device):
    return pltpu.make_async_remote_copy(
        src_ref=src, dst_ref=dst, send_sem=send_sem, recv_sem=recv_sem,
        device_id=device, device_id_type=MESH,
    )


def gather_kernel(
    parts, chips, q_width, kv_width, first_kv_of,
    x_ref, wq_ref, wk_ref, wv_ref, rows_ref, cols_ref,
    stage, x_send, x_recv, own_sem, stage_sem,
    up_send, up_recv, down_send, down_recv, pair_send, pair_recv,
):
    sp, dp = lax.axis_index("sp"), lax.axis_index("dp")
    z, core = dp // 2, dp % 2
    partner = z * 2 + (1 - core)
    row_count = x_ref.shape[0]
    depth = stage.shape[0]
    square = parts == 4

    first_kv = first_kv_of(sp)
    loads = [
        pltpu.make_async_copy(
            wq_ref.at[:, pl.ds(pl.multiple_of(sp * q_width, 128), q_width)],
            stage.at[:, pl.ds(0, q_width)], stage_sem.at[0]),
        pltpu.make_async_copy(
            wk_ref.at[:, pl.ds(pl.multiple_of(first_kv * HEAD_WIDTH, 128), kv_width)],
            stage.at[:, pl.ds(q_width, kv_width)], stage_sem.at[1]),
        pltpu.make_async_copy(
            wv_ref.at[:, pl.ds(pl.multiple_of(first_kv * HEAD_WIDTH, 128), kv_width)],
            stage.at[:, pl.ds(q_width + kv_width, kv_width)], stage_sem.at[2]),
    ]
    for load in loads:
        load.start()

    barrier = pltpu.get_barrier_semaphore()
    if square:
        x_side = (sp // 2) * 2 + (1 - sp % 2)
        y_side = (1 - sp // 2) * 2 + sp % 2
        corner = (1 - sp // 2) * 2 + (1 - sp % 2)
        greeted = [x_side, y_side]
    else:
        greeted = [lax.rem(sp + i, parts) for i in range(1, parts)]
    for peer in greeted:
        pl.semaphore_signal(barrier, inc=1, device_id={"sp": peer, "dp": dp}, device_id_type=MESH)
    pl.semaphore_signal(barrier, inc=1, device_id={"sp": sp, "dp": partner}, device_id_type=MESH)

    @pl.when(z < chips - 1)
    def _():
        pl.semaphore_signal(barrier, inc=1, device_id={"sp": sp, "dp": dp + 2}, device_id_type=MESH)

    @pl.when(z > 0)
    def _():
        pl.semaphore_signal(barrier, inc=1, device_id={"sp": sp, "dp": dp - 2}, device_id_type=MESH)

    in_chain = (z + chips - 1) // chips + (2 * chips - 2 - z) // chips
    pl.semaphore_wait(barrier, len(greeted) + 1 + in_chain)

    def token_rows(owner, half=None):
        if half is None:
            return rows_ref.at[pl.ds(owner * row_count, row_count)]
        return rows_ref.at[pl.ds(owner * row_count + half * (row_count // 2), row_count // 2)]

    token_sends = []
    if square:
        for half_x, half_y in ((0, 1), (1, 0)):
            for slot, half, peer in ((0, half_x, x_side), (1, half_y, y_side)):
                copy = remote(
                    x_ref.at[pl.ds(half * (row_count // 2), row_count // 2)],
                    token_rows(sp, half), x_send.at[slot * 2 + half],
                    x_recv.at[slot * 2 + half], {"sp": peer, "dp": dp})
                copy.start()
                token_sends.append(copy)
    else:
        for i, peer in enumerate(greeted):
            copy = remote(
                x_ref, token_rows(sp), x_send.at[i], x_recv.at[i], {"sp": peer, "dp": dp})
            copy.start()
            token_sends.append(copy)
    own_rows = pltpu.make_async_copy(x_ref, token_rows(sp), own_sem.at[0])
    own_rows.start()

    for load in loads:
        load.wait()

    def block(owner_z, owner_core):
        return cols_ref.at[pl.ds((owner_z * 2 + owner_core) * depth, depth)]

    def to_up(src, k):
        return remote(src, block(z - k, core), up_send.at[k], up_recv.at[k + 1],
                      {"sp": sp, "dp": dp + 2})

    def to_down(src, k):
        return remote(src, block(z + k, core), down_send.at[k], down_recv.at[k + 1],
                      {"sp": sp, "dp": dp - 2})

    def to_pair(src, owner_z):
        return remote(src, block(owner_z, core), pair_send.at[owner_z], pair_recv.at[owner_z],
                      {"sp": sp, "dp": partner})

    @pl.when(z < chips - 1)
    def _():
        to_up(stage, 0).start()

    @pl.when(z > 0)
    def _():
        to_down(stage, 0).start()

    to_pair(stage, z).start()
    own_cols = pltpu.make_async_copy(stage, block(z, core), own_sem.at[1])
    own_cols.start()

    if square:
        got_x = remote(x_ref.at[pl.ds(0, row_count // 2)], token_rows(x_side, 0),
                       x_send.at[0], x_recv.at[0], {"sp": x_side, "dp": dp})
        got_y = remote(x_ref.at[pl.ds(0, row_count // 2)], token_rows(y_side, 1),
                       x_send.at[3], x_recv.at[3], {"sp": y_side, "dp": dp})

    def relay_columns(k):
        @pl.when(z >= k)
        def _():
            source = block(z - k, core)
            remote(source, source, up_send.at[k], up_recv.at[k], {"sp": sp, "dp": partner}).wait_recv()
            if k < chips - 1:
                @pl.when(z < chips - 1)
                def _():
                    to_up(source, k).start()
            to_pair(source, z - k).start()

        @pl.when(z + k <= chips - 1)
        def _():
            source = block(z + k, core)
            remote(source, source, down_send.at[k], down_recv.at[k], {"sp": sp, "dp": partner}).wait_recv()
            if k < chips - 1:
                @pl.when(z > 0)
                def _():
                    to_down(source, k).start()
            to_pair(source, z + k).start()

    if chips > 1:
        relay_columns(1)
    if square:
        got_x.wait_recv()
        relay_x = remote(token_rows(x_side, 0), token_rows(x_side, 0),
                         x_send.at[4], x_recv.at[4], {"sp": y_side, "dp": dp})
        relay_x.start()
        got_y.wait_recv()
        relay_y = remote(token_rows(y_side, 1), token_rows(y_side, 1),
                         x_send.at[5], x_recv.at[5], {"sp": x_side, "dp": dp})
        relay_y.start()
        token_sends += [relay_x, relay_y]
    for k in range(2, chips):
        relay_columns(k)

    for owner_z in range(chips):
        source = block(owner_z, 1 - core)
        remote(source, source, pair_send.at[owner_z], pair_recv.at[owner_z],
               {"sp": sp, "dp": partner}).wait_recv()
    if square:
        for owner, half, slot in (
            (x_side, 1, 1), (y_side, 0, 2), (corner, 0, 4), (corner, 1, 5)
        ):
            target = token_rows(owner, half)
            remote(target, target, x_send.at[slot], x_recv.at[slot],
                   {"sp": x_side, "dp": dp}).wait_recv()
    else:
        for i in range(parts - 1):
            target = token_rows(lax.rem(sp + parts - 1 - i, parts))
            remote(target, target, x_send.at[i], x_recv.at[i],
                   {"sp": greeted[0], "dp": dp}).wait_recv()
    for copy in token_sends:
        copy.wait_send()
    for owner_z in range(chips):
        to_pair(stage, owner_z).wait_send()
    for k in range(chips - 1):
        @pl.when(jnp.logical_and(z < chips - 1, z >= k))
        def _():
            to_up(stage, k).wait_send()

        @pl.when(jnp.logical_and(z > 0, z + k <= chips - 1))
        def _():
            to_down(stage, k).wait_send()
    own_rows.wait()
    own_cols.wait()


def gather(sequence, query_weight, key_weight, value_matrix, parts, chips, q_width, kv_width, first_kv_of):
    depth, width = query_weight.shape[0], q_width + 2 * kv_width
    row_count, features = sequence.shape
    dma = pltpu.SemaphoreType.DMA
    chain = dma((chips + 1,))
    return pl.pallas_call(
        functools.partial(gather_kernel, parts, chips, q_width, kv_width, first_kv_of),
        out_shape=(
            jax.ShapeDtypeStruct((parts * row_count, features), jnp.bfloat16),
            jax.ShapeDtypeStruct((chips * 2 * depth, width), jnp.bfloat16),
        ),
        in_specs=[pl.BlockSpec(memory_space=pltpu.VMEM), ANY, ANY, ANY],
        out_specs=(ANY, ANY),
        scratch_shapes=[
            pltpu.VMEM((depth, width), jnp.bfloat16),
            dma((max(6, parts),)), dma((max(6, parts),)), dma((2,)), dma((3,)),
            chain, chain, chain, chain, chain, chain,
        ],
        compiler_params=pltpu.CompilerParams(collective_id=0, has_side_effects=True),
        cost_estimate=pl.CostEstimate(flops=40_000_000_000, bytes_accessed=100_000_000, transcendentals=0),
        name="gather_rows_columns",
    )(sequence, query_weight, key_weight, value_matrix)


def exchange_kernel(parts, a_ref, o_ref, send, recv, own_sem):
    sp, dp = lax.axis_index("sp"), lax.axis_index("dp")
    row_count = o_ref.shape[1]
    barrier = pltpu.get_barrier_semaphore()
    peers = [lax.rem(sp + i, parts) for i in range(1, parts)]
    for peer in peers:
        pl.semaphore_signal(barrier, inc=1, device_id={"sp": peer, "dp": dp}, device_id_type=MESH)
    pl.semaphore_wait(barrier, parts - 1)
    copies = []
    for i, peer in enumerate(peers):
        copy = remote(a_ref.at[pl.ds(peer * row_count, row_count)], o_ref.at[sp],
                      send.at[i], recv.at[i], {"sp": peer, "dp": dp})
        copy.start()
        copies.append(copy)
    own = pltpu.make_async_copy(a_ref.at[pl.ds(sp * row_count, row_count)], o_ref.at[sp], own_sem)
    own.start()
    for i in range(parts - 1):
        target = o_ref.at[lax.rem(sp + parts - 1 - i, parts)]
        remote(target, target, send.at[i], recv.at[i], {"sp": peers[0], "dp": dp}).wait_recv()
    for copy in copies:
        copy.wait_send()
    own.wait()


def exchange(attended, parts):
    length, width = attended.shape
    row_count = length // parts
    dma = pltpu.SemaphoreType.DMA
    return pl.pallas_call(
        functools.partial(exchange_kernel, parts),
        out_shape=jax.ShapeDtypeStruct((parts, row_count, width), jnp.bfloat16),
        in_specs=[pl.BlockSpec(memory_space=pltpu.VMEM)],
        out_specs=ANY,
        scratch_shapes=[dma((parts,)), dma((parts,)), dma],
        compiler_params=pltpu.CompilerParams(collective_id=1, has_side_effects=True),
        cost_estimate=pl.CostEstimate(flops=10_000_000_000, bytes_accessed=20_000_000, transcendentals=0),
        name="exchange_heads",
    )(attended)


def project_kernel(q_heads, kv_heads, x_ref, g_ref, w_ref, qg_ref, kg_ref, cos_ref, sin_ref,
                   q_ref, k_ref, v_ref):
    x = x_ref[...].astype(jnp.float32)
    scale = lax.rsqrt(jnp.mean(x * x, axis=-1, keepdims=True) + EPS)
    normed = (x * scale * g_ref[...]).astype(jnp.bfloat16)
    mixed = jnp.dot(normed, w_ref[...], preferred_element_type=jnp.float32)
    cosine, sine = cos_ref[...], sin_ref[...]
    lane = lax.broadcasted_iota(jnp.int32, cosine.shape, 1)
    first = lane % (HEAD_WIDTH // 2) < HEAD_WIDTH // 4

    def finish(head, gain):
        head = head * lax.rsqrt(jnp.mean(head * head, axis=-1, keepdims=True) + EPS) * gain
        other = jnp.where(first, pltpu.roll(head, HEAD_WIDTH - HEAD_WIDTH // 4, 1),
                          pltpu.roll(head, HEAD_WIDTH // 4, 1))
        return (head * cosine + other * sine).astype(jnp.bfloat16)

    for h in range(q_heads):
        span = slice(h * HEAD_WIDTH, (h + 1) * HEAD_WIDTH)
        q_ref[:, span] = finish(mixed[:, span], qg_ref[...])
    for h in range(kv_heads):
        span = slice(h * HEAD_WIDTH, (h + 1) * HEAD_WIDTH)
        start = (q_heads + h) * HEAD_WIDTH
        k_ref[:, span] = finish(mixed[:, start:start + HEAD_WIDTH], kg_ref[...])
    v_ref[...] = mixed[:, (q_heads + kv_heads) * HEAD_WIDTH:].astype(jnp.bfloat16)


def project(rows, in_gain, columns, query_gain, key_gain, cosine, sine, q_heads, kv_heads, row_block):
    length, features = rows.shape
    width = columns.shape[1]
    q_width, kv_width = q_heads * HEAD_WIDTH, kv_heads * HEAD_WIDTH
    whole = lambda shape: pl.BlockSpec(shape, lambda i: (0, 0))
    part = lambda size: pl.BlockSpec((row_block, size), lambda i: (i, 0))
    return pl.pallas_call(
        functools.partial(project_kernel, q_heads, kv_heads),
        grid=(length // row_block,),
        out_shape=tuple(jax.ShapeDtypeStruct((length, n), jnp.bfloat16) for n in (q_width, kv_width, kv_width)),
        in_specs=[part(features), whole((1, features)), whole((features, width)),
                  whole((1, HEAD_WIDTH)), whole((1, HEAD_WIDTH)), part(HEAD_WIDTH), part(HEAD_WIDTH)],
        out_specs=(part(q_width), part(kv_width), part(kv_width)),
        cost_estimate=pl.CostEstimate(flops=2 * length * features * width, bytes_accessed=9_000_000, transcendentals=0),
        name="project_heads",
    )(rows, in_gain[None], columns, query_gain[None], key_gain[None], cosine, sine)


def attend_kernel(q_ref, k_ref, v_ref, o_ref):
    factor = HEAD_WIDTH ** (-0.5) * float(np.log2(np.e))
    scores = lax.dot_general(q_ref[...], k_ref[...], (((1,), (1,)), ((), ())),
                             preferred_element_type=jnp.float32)
    top = jnp.max(scores, axis=-1, keepdims=True)
    raised = jnp.exp2((scores - top) * factor)
    weights = (raised * (1.0 / jnp.sum(raised, axis=-1, keepdims=True))).astype(jnp.bfloat16)
    o_ref[...] = jnp.dot(weights, v_ref[...], preferred_element_type=jnp.float32).astype(jnp.bfloat16)


def attend(q, k, v, q_heads, kv_heads, row_block):
    length = q.shape[0]
    group = q_heads // kv_heads
    block = pl.BlockSpec((row_block, HEAD_WIDTH), lambda h, i: (i, h))
    keys = pl.BlockSpec((length, HEAD_WIDTH), lambda h, i: (0, h // group))
    return pl.pallas_call(
        attend_kernel,
        grid=(q_heads, length // row_block),
        out_shape=jax.ShapeDtypeStruct(q.shape, jnp.bfloat16),
        in_specs=[block, keys, keys],
        out_specs=block,
        cost_estimate=pl.CostEstimate(flops=4 * length * length * q_heads * HEAD_WIDTH,
                                      bytes_accessed=3_000_000, transcendentals=length * length * q_heads),
        name="attend_heads",
    )(q, k, v)


def output_kernel(a_ref, w_ref, g_ref, o_ref, total):
    step = pl.program_id(0)
    product = jnp.dot(a_ref[0], w_ref[...], preferred_element_type=jnp.float32)

    @pl.when(step == 0)
    def _():
        total[...] = product

    @pl.when(step > 0)
    def _():
        total[...] += product

    @pl.when(step == pl.num_programs(0) - 1)
    def _():
        x = total[...]
        scale = lax.rsqrt(jnp.mean(x * x, axis=-1, keepdims=True) + EPS)
        o_ref[...] = (x * scale * g_ref[...]).astype(jnp.bfloat16)


def output(returned, out_weight, out_gain):
    parts, row_count, width = returned.shape
    features = out_weight.shape[1]
    return pl.pallas_call(
        output_kernel,
        grid=(parts,),
        out_shape=jax.ShapeDtypeStruct((row_count, features), jnp.bfloat16),
        in_specs=[pl.BlockSpec((1, row_count, width), lambda s: (s, 0, 0)),
                  pl.BlockSpec((width, features), lambda s: (s, 0)),
                  pl.BlockSpec((1, features), lambda s: (0, 0))],
        out_specs=pl.BlockSpec((row_count, features), lambda s: (0, 0)),
        scratch_shapes=[pltpu.VMEM((row_count, features), jnp.float32)],
        cost_estimate=pl.CostEstimate(flops=2 * row_count * features * width * parts,
                                      bytes_accessed=10_000_000, transcendentals=0),
        name="output_rows",
    )(returned, out_weight, out_gain[None])


def rotation(length):
    quarter = HEAD_WIDTH // 4
    inverse_freq = (THETA ** (-np.arange(quarter, dtype=np.float32) / quarter)).astype(np.float32)

    def table(count):
        angle = (np.arange(count, dtype=np.float32)[:, None] * inverse_freq[None, :]).astype(np.float64)
        cosine, sine = np.cos(angle), np.sin(angle)
        return (np.concatenate([cosine, cosine], 1).astype(np.float32),
                np.concatenate([-sine, sine], 1).astype(np.float32))

    rows = -(-length // GRID_W)
    row_tables, col_tables = table(rows), table(GRID_W)
    half = HEAD_WIDTH // 2
    out = []
    for row, col in zip(row_tables, col_tables):
        row = jnp.broadcast_to(jnp.asarray(row)[:, None, :], (rows, GRID_W, half))
        col = jnp.broadcast_to(jnp.asarray(col)[None, :, :], (rows, GRID_W, half))
        out.append(jnp.concatenate([row, col], -1).reshape(rows * GRID_W, HEAD_WIDTH)[:length])
    return out


def on_device(parts, groups, tokens, in_gain, query_weight, key_weight, value_matrix,
              query_gain, key_gain, out_weight, out_gain):
    sequence = tokens[0]
    row_count = sequence.shape[0]
    q_heads = QUERY_HEAD_COUNT // parts
    kv_heads = max(1, KEY_VALUE_HEADS // parts)
    per_group = QUERY_HEAD_COUNT // KEY_VALUE_HEADS
    out_full = lax.all_gather(out_weight, "dp", axis=0, tiled=True)
    cosine, sine = rotation(parts * row_count)
    rows, columns = gather(
        sequence, query_weight, key_weight, value_matrix, parts, groups // 2,
        q_heads * HEAD_WIDTH, kv_heads * HEAD_WIDTH, lambda sp: sp * q_heads // per_group)
    q, k, v = project(rows, in_gain, columns, query_gain, key_gain, cosine, sine, q_heads, kv_heads, row_count)
    attended = attend(q, k, v, q_heads, kv_heads, row_count)
    returned = exchange(attended, parts)
    return output(returned, out_full, out_gain)[None]


def solution(mesh):
    placed = (P("dp", "sp", None), P(), P("dp", None), P("dp", None), P("dp", None),
              P(), P(), P("dp", None), P())
    return jax.shard_map(
        functools.partial(on_device, mesh.shape["sp"], mesh.shape["dp"]),
        mesh=mesh, in_specs=placed, out_specs=P("dp", "sp", None), check_vma=False,
    )
```

```python
import functools

import jax
import jax.numpy as jnp
import numpy as np
from jax import lax
from jax.experimental import pallas as pl
from jax.experimental.pallas import tpu as pltpu
from jax.sharding import PartitionSpec as P

QUERY_HEAD_COUNT = 16
KEY_VALUE_HEADS = 4
HEAD_WIDTH = 128
GRID_W = 64
EPS = 1e-06
THETA = 10000.0
MESH = pl.DeviceIdType.MESH
ANY = pl.BlockSpec(memory_space=pl.ANY)


def remote(src, dst, send_sem, recv_sem, device):
    return pltpu.make_async_remote_copy(
        src_ref=src, dst_ref=dst, send_sem=send_sem, recv_sem=recv_sem,
        device_id=device, device_id_type=MESH,
    )


def gather_kernel(
    parts, chips, q_width, kv_width, first_kv_of,
    x_ref, wq_ref, wk_ref, wv_ref, wo_ref, rows_ref, cols_ref, head_ref, tail_ref,
    stage, x_send, x_recv, own_sem, stage_sem,
    up_send, up_recv, down_send, down_recv, pair_send, pair_recv,
):
    sp, dp = lax.axis_index("sp"), lax.axis_index("dp")
    z, core = dp // 2, dp % 2
    partner = z * 2 + (1 - core)
    row_count = x_ref.shape[0]
    depth = stage.shape[0]
    square = parts == 4

    first_kv = first_kv_of(sp)
    loads = [
        pltpu.make_async_copy(
            wq_ref.at[:, pl.ds(pl.multiple_of(sp * q_width, 128), q_width)],
            stage.at[:, pl.ds(0, q_width)], stage_sem.at[0]),
        pltpu.make_async_copy(
            wk_ref.at[:, pl.ds(pl.multiple_of(first_kv * HEAD_WIDTH, 128), kv_width)],
            stage.at[:, pl.ds(q_width, kv_width)], stage_sem.at[1]),
        pltpu.make_async_copy(
            wv_ref.at[:, pl.ds(pl.multiple_of(first_kv * HEAD_WIDTH, 128), kv_width)],
            stage.at[:, pl.ds(q_width + kv_width, kv_width)], stage_sem.at[2]),
    ]
    for load in loads:
        load.start()

    barrier = pltpu.get_barrier_semaphore()
    if square:
        x_side = (sp // 2) * 2 + (1 - sp % 2)
        y_side = (1 - sp // 2) * 2 + sp % 2
        corner = (1 - sp // 2) * 2 + (1 - sp % 2)
        greeted = [x_side, y_side]
    else:
        greeted = [lax.rem(sp + i, parts) for i in range(1, parts)]
    for peer in greeted:
        pl.semaphore_signal(barrier, inc=1, device_id={"sp": peer, "dp": dp}, device_id_type=MESH)
    pl.semaphore_signal(barrier, inc=1, device_id={"sp": sp, "dp": partner}, device_id_type=MESH)

    @pl.when(z < chips - 1)
    def _():
        pl.semaphore_signal(barrier, inc=1, device_id={"sp": sp, "dp": dp + 2}, device_id_type=MESH)

    @pl.when(z > 0)
    def _():
        pl.semaphore_signal(barrier, inc=1, device_id={"sp": sp, "dp": dp - 2}, device_id_type=MESH)

    in_chain = (z + chips - 1) // chips + (2 * chips - 2 - z) // chips
    pl.semaphore_wait(barrier, len(greeted) + 1 + in_chain)

    def token_rows(owner, half=None):
        if half is None:
            return rows_ref.at[pl.ds(owner * row_count, row_count)]
        return rows_ref.at[pl.ds(owner * row_count + half * (row_count // 2), row_count // 2)]

    token_sends = []
    if square:
        for half_x, half_y in ((0, 1), (1, 0)):
            for slot, half, peer in ((0, half_x, x_side), (1, half_y, y_side)):
                copy = remote(
                    x_ref.at[pl.ds(half * (row_count // 2), row_count // 2)],
                    token_rows(sp, half), x_send.at[slot * 2 + half],
                    x_recv.at[slot * 2 + half], {"sp": peer, "dp": dp})
                copy.start()
                token_sends.append(copy)
    else:
        for i, peer in enumerate(greeted):
            copy = remote(
                x_ref, token_rows(sp), x_send.at[i], x_recv.at[i], {"sp": peer, "dp": dp})
            copy.start()
            token_sends.append(copy)
    own_rows = pltpu.make_async_copy(x_ref, token_rows(sp), own_sem.at[0])
    own_rows.start()
    split = head_ref.shape[1]
    out_head = wo_ref.at[:, pl.ds(0, split)]
    own_tail = pltpu.make_async_copy(
        wo_ref.at[:, pl.ds(split, tail_ref.shape[1])], tail_ref, own_sem.at[2])
    own_tail.start()

    for load in loads:
        load.wait()

    gathered = (cols_ref, head_ref)
    sources = (stage, out_head)

    def block(t, owner_z, owner_core):
        return gathered[t].at[pl.ds((owner_z * 2 + owner_core) * depth, depth)]

    def to_up(t, src, k):
        return remote(src, block(t, z - k, core), up_send.at[t, k], up_recv.at[t, k + 1],
                      {"sp": sp, "dp": dp + 2})

    def to_down(t, src, k):
        return remote(src, block(t, z + k, core), down_send.at[t, k], down_recv.at[t, k + 1],
                      {"sp": sp, "dp": dp - 2})

    def to_pair(t, src, owner_z):
        return remote(src, block(t, owner_z, core), pair_send.at[t, owner_z],
                      pair_recv.at[t, owner_z], {"sp": sp, "dp": partner})

    own_copies = []
    for t in range(2):
        @pl.when(z < chips - 1)
        def _():
            to_up(t, sources[t], 0).start()

        @pl.when(z > 0)
        def _():
            to_down(t, sources[t], 0).start()

        to_pair(t, sources[t], z).start()
        own = pltpu.make_async_copy(sources[t], block(t, z, core), own_sem.at[(1, 3)[t]])
        own.start()
        own_copies.append(own)

    if square:
        got_x = remote(x_ref.at[pl.ds(0, row_count // 2)], token_rows(x_side, 0),
                       x_send.at[0], x_recv.at[0], {"sp": x_side, "dp": dp})
        got_y = remote(x_ref.at[pl.ds(0, row_count // 2)], token_rows(y_side, 1),
                       x_send.at[3], x_recv.at[3], {"sp": y_side, "dp": dp})

    def relay_columns(t, k):
        @pl.when(z >= k)
        def _():
            source = block(t, z - k, core)
            remote(source, source, up_send.at[t, k], up_recv.at[t, k],
                   {"sp": sp, "dp": partner}).wait_recv()
            if k < chips - 1:
                @pl.when(z < chips - 1)
                def _():
                    to_up(t, source, k).start()
            to_pair(t, source, z - k).start()

        @pl.when(z + k <= chips - 1)
        def _():
            source = block(t, z + k, core)
            remote(source, source, down_send.at[t, k], down_recv.at[t, k],
                   {"sp": sp, "dp": partner}).wait_recv()
            if k < chips - 1:
                @pl.when(z > 0)
                def _():
                    to_down(t, source, k).start()
            to_pair(t, source, z + k).start()

    if chips > 1:
        relay_columns(0, 1)
    if square:
        got_x.wait_recv()
        relay_x = remote(token_rows(x_side, 0), token_rows(x_side, 0),
                         x_send.at[4], x_recv.at[4], {"sp": y_side, "dp": dp})
        relay_x.start()
        got_y.wait_recv()
        relay_y = remote(token_rows(y_side, 1), token_rows(y_side, 1),
                         x_send.at[5], x_recv.at[5], {"sp": x_side, "dp": dp})
        relay_y.start()
        token_sends += [relay_x, relay_y]
    for k in range(1, chips):
        if k > 1:
            relay_columns(0, k)
        relay_columns(1, k)

    for t in range(2):
        for owner_z in range(chips):
            source = block(t, owner_z, 1 - core)
            remote(source, source, pair_send.at[t, owner_z], pair_recv.at[t, owner_z],
                   {"sp": sp, "dp": partner}).wait_recv()
    if square:
        for owner, half, slot in (
            (x_side, 1, 1), (y_side, 0, 2), (corner, 0, 4), (corner, 1, 5)
        ):
            target = token_rows(owner, half)
            remote(target, target, x_send.at[slot], x_recv.at[slot],
                   {"sp": x_side, "dp": dp}).wait_recv()
    else:
        for i in range(parts - 1):
            target = token_rows(lax.rem(sp + parts - 1 - i, parts))
            remote(target, target, x_send.at[i], x_recv.at[i],
                   {"sp": greeted[0], "dp": dp}).wait_recv()
    for copy in token_sends:
        copy.wait_send()
    for t in range(2):
        for owner_z in range(chips):
            to_pair(t, sources[t], owner_z).wait_send()
        for k in range(chips - 1):
            @pl.when(jnp.logical_and(z < chips - 1, z >= k))
            def _():
                to_up(t, sources[t], k).wait_send()

            @pl.when(jnp.logical_and(z > 0, z + k <= chips - 1))
            def _():
                to_down(t, sources[t], k).wait_send()
    own_rows.wait()
    own_tail.wait()
    for own in own_copies:
        own.wait()


def gather(sequence, query_weight, key_weight, value_matrix, out_weight, parts, chips, q_width, kv_width, first_kv_of):
    depth, width = query_weight.shape[0], q_width + 2 * kv_width
    row_count, features = sequence.shape
    dma = pltpu.SemaphoreType.DMA
    chain = dma((2, chips + 1))
    split = out_weight.shape[1] // 2
    return pl.pallas_call(
        functools.partial(gather_kernel, parts, chips, q_width, kv_width, first_kv_of),
        out_shape=(
            jax.ShapeDtypeStruct((parts * row_count, features), jnp.bfloat16),
            jax.ShapeDtypeStruct((chips * 2 * depth, width), jnp.bfloat16),
            jax.ShapeDtypeStruct((chips * 2 * depth, split), jnp.bfloat16),
            jax.ShapeDtypeStruct((depth, out_weight.shape[1] - split), jnp.bfloat16),
        ),
        in_specs=[pl.BlockSpec(memory_space=pltpu.VMEM), ANY, ANY, ANY,
                  pl.BlockSpec(memory_space=pltpu.VMEM)],
        out_specs=(ANY, ANY, ANY, ANY),
        scratch_shapes=[
            pltpu.VMEM((depth, width), jnp.bfloat16),
            dma((max(6, parts),)), dma((max(6, parts),)), dma((4,)), dma((3,)),
            chain, chain, chain, chain, chain, chain,
        ],
        compiler_params=pltpu.CompilerParams(collective_id=0, has_side_effects=True),
        cost_estimate=pl.CostEstimate(flops=40_000_000_000, bytes_accessed=100_000_000, transcendentals=0),
        name="gather_rows_columns",
    )(sequence, query_weight, key_weight, value_matrix, out_weight)


def exchange_kernel(parts, a_ref, o_ref, send, recv, own_sem):
    sp, dp = lax.axis_index("sp"), lax.axis_index("dp")
    row_count = o_ref.shape[1]
    barrier = pltpu.get_barrier_semaphore()
    peers = [lax.rem(sp + i, parts) for i in range(1, parts)]
    for peer in peers:
        pl.semaphore_signal(barrier, inc=1, device_id={"sp": peer, "dp": dp}, device_id_type=MESH)
    pl.semaphore_wait(barrier, parts - 1)
    copies = []
    for i, peer in enumerate(peers):
        copy = remote(a_ref.at[pl.ds(peer * row_count, row_count)], o_ref.at[sp],
                      send.at[i], recv.at[i], {"sp": peer, "dp": dp})
        copy.start()
        copies.append(copy)
    own = pltpu.make_async_copy(a_ref.at[pl.ds(sp * row_count, row_count)], o_ref.at[sp], own_sem)
    own.start()
    for i in range(parts - 1):
        target = o_ref.at[lax.rem(sp + parts - 1 - i, parts)]
        remote(target, target, send.at[i], recv.at[i], {"sp": peers[0], "dp": dp}).wait_recv()
    for copy in copies:
        copy.wait_send()
    own.wait()


def exchange(attended, parts):
    length, width = attended.shape
    row_count = length // parts
    dma = pltpu.SemaphoreType.DMA
    return pl.pallas_call(
        functools.partial(exchange_kernel, parts),
        out_shape=jax.ShapeDtypeStruct((parts, row_count, width), jnp.bfloat16),
        in_specs=[pl.BlockSpec(memory_space=pltpu.VMEM)],
        out_specs=ANY,
        scratch_shapes=[dma((parts,)), dma((parts,)), dma],
        compiler_params=pltpu.CompilerParams(collective_id=1, has_side_effects=True),
        cost_estimate=pl.CostEstimate(flops=10_000_000_000, bytes_accessed=20_000_000, transcendentals=0),
        name="exchange_heads",
    )(attended)


def project_kernel(q_heads, kv_heads, x_ref, g_ref, w_ref, qg_ref, kg_ref, cos_ref, sin_ref,
                   q_ref, k_ref, v_ref):
    x = x_ref[...].astype(jnp.float32)
    scale = lax.rsqrt(jnp.mean(x * x, axis=-1, keepdims=True) + EPS)
    normed = (x * scale * g_ref[...]).astype(jnp.bfloat16)
    mixed = jnp.dot(normed, w_ref[...], preferred_element_type=jnp.float32)
    cosine, sine = cos_ref[...], sin_ref[...]
    lane = lax.broadcasted_iota(jnp.int32, cosine.shape, 1)
    first = lane % (HEAD_WIDTH // 2) < HEAD_WIDTH // 4

    def finish(head, gain):
        head = head * lax.rsqrt(jnp.mean(head * head, axis=-1, keepdims=True) + EPS) * gain
        other = jnp.where(first, pltpu.roll(head, HEAD_WIDTH - HEAD_WIDTH // 4, 1),
                          pltpu.roll(head, HEAD_WIDTH // 4, 1))
        return (head * cosine + other * sine).astype(jnp.bfloat16)

    for h in range(q_heads):
        span = slice(h * HEAD_WIDTH, (h + 1) * HEAD_WIDTH)
        q_ref[:, span] = finish(mixed[:, span], qg_ref[...])
    for h in range(kv_heads):
        span = slice(h * HEAD_WIDTH, (h + 1) * HEAD_WIDTH)
        start = (q_heads + h) * HEAD_WIDTH
        k_ref[:, span] = finish(mixed[:, start:start + HEAD_WIDTH], kg_ref[...])
    v_ref[...] = mixed[:, (q_heads + kv_heads) * HEAD_WIDTH:].astype(jnp.bfloat16)


def project(rows, in_gain, columns, query_gain, key_gain, cosine, sine, q_heads, kv_heads, row_block):
    length, features = rows.shape
    width = columns.shape[1]
    q_width, kv_width = q_heads * HEAD_WIDTH, kv_heads * HEAD_WIDTH
    whole = lambda shape: pl.BlockSpec(shape, lambda i: (0, 0))
    part = lambda size: pl.BlockSpec((row_block, size), lambda i: (i, 0))
    return pl.pallas_call(
        functools.partial(project_kernel, q_heads, kv_heads),
        grid=(length // row_block,),
        out_shape=tuple(jax.ShapeDtypeStruct((length, n), jnp.bfloat16) for n in (q_width, kv_width, kv_width)),
        in_specs=[part(features), whole((1, features)), whole((features, width)),
                  whole((1, HEAD_WIDTH)), whole((1, HEAD_WIDTH)), part(HEAD_WIDTH), part(HEAD_WIDTH)],
        out_specs=(part(q_width), part(kv_width), part(kv_width)),
        cost_estimate=pl.CostEstimate(flops=2 * length * features * width, bytes_accessed=9_000_000, transcendentals=0),
        name="project_heads",
    )(rows, in_gain[None], columns, query_gain[None], key_gain[None], cosine, sine)


def attend_kernel(group, q_ref, k_ref, v_ref, o_ref):
    factor = HEAD_WIDTH ** (-0.5) * float(np.log2(np.e))
    for h in range(q_ref.shape[1] // HEAD_WIDTH):
        span = slice(h * HEAD_WIDTH, (h + 1) * HEAD_WIDTH)
        shared = slice(h // group * HEAD_WIDTH, (h // group + 1) * HEAD_WIDTH)
        scores = lax.dot_general(q_ref[:, span], k_ref[:, shared], (((1,), (1,)), ((), ())),
                                 preferred_element_type=jnp.float32)
        top = jnp.max(scores, axis=-1, keepdims=True)
        raised = jnp.exp2((scores - top) * factor)
        weights = (raised * (1.0 / jnp.sum(raised, axis=-1, keepdims=True))).astype(jnp.bfloat16)
        o_ref[:, span] = jnp.dot(
            weights, v_ref[:, shared], preferred_element_type=jnp.float32).astype(jnp.bfloat16)


def attend(q, k, v, q_heads, kv_heads, row_block):
    length = q.shape[0]
    block = pl.BlockSpec((row_block, q.shape[1]), lambda i: (i, 0))
    keys = pl.BlockSpec(k.shape, lambda i: (0, 0))
    return pl.pallas_call(
        functools.partial(attend_kernel, q_heads // kv_heads),
        grid=(length // row_block,),
        out_shape=jax.ShapeDtypeStruct(q.shape, jnp.bfloat16),
        in_specs=[block, keys, keys],
        out_specs=block,
        cost_estimate=pl.CostEstimate(flops=4 * length * length * q_heads * HEAD_WIDTH,
                                      bytes_accessed=3_000_000, transcendentals=length * length * q_heads),
        name="attend_heads",
    )(q, k, v)


def output_kernel(a_ref, head_ref, tail_ref, g_ref, o_ref, total):
    step = pl.program_id(0)
    split = head_ref.shape[1]

    @pl.when(step == 0)
    def _():
        total[...] = jnp.zeros_like(total)

    total[:, :split] += jnp.dot(a_ref[0], head_ref[...], preferred_element_type=jnp.float32)
    total[:, split:] += jnp.dot(a_ref[0], tail_ref[...], preferred_element_type=jnp.float32)

    @pl.when(step == pl.num_programs(0) - 1)
    def _():
        x = total[...]
        scale = lax.rsqrt(jnp.mean(x * x, axis=-1, keepdims=True) + EPS)
        o_ref[...] = (x * scale * g_ref[...]).astype(jnp.bfloat16)


def output(returned, out_head, out_tail, out_gain):
    parts, row_count, width = returned.shape
    features = out_gain.shape[0]
    split = out_head.shape[1]
    return pl.pallas_call(
        output_kernel,
        grid=(parts,),
        out_shape=jax.ShapeDtypeStruct((row_count, features), jnp.bfloat16),
        in_specs=[pl.BlockSpec((1, row_count, width), lambda s: (s, 0, 0)),
                  pl.BlockSpec((width, split), lambda s: (s, 0)),
                  pl.BlockSpec((width, features - split), lambda s: (s, 0)),
                  pl.BlockSpec((1, features), lambda s: (0, 0))],
        out_specs=pl.BlockSpec((row_count, features), lambda s: (0, 0)),
        scratch_shapes=[pltpu.VMEM((row_count, features), jnp.float32)],
        cost_estimate=pl.CostEstimate(flops=2 * row_count * features * width * parts,
                                      bytes_accessed=10_000_000, transcendentals=0),
        name="output_rows",
    )(returned, out_head, out_tail, out_gain[None])


def rotation(length):
    quarter = HEAD_WIDTH // 4
    inverse_freq = (THETA ** (-np.arange(quarter, dtype=np.float32) / quarter)).astype(np.float32)

    def table(count):
        angle = (np.arange(count, dtype=np.float32)[:, None] * inverse_freq[None, :]).astype(np.float64)
        cosine, sine = np.cos(angle), np.sin(angle)
        return (np.concatenate([cosine, cosine], 1).astype(np.float32),
                np.concatenate([-sine, sine], 1).astype(np.float32))

    rows = -(-length // GRID_W)
    row_tables, col_tables = table(rows), table(GRID_W)
    half = HEAD_WIDTH // 2
    out = []
    for row, col in zip(row_tables, col_tables):
        row = np.broadcast_to(row[:, None, :], (rows, GRID_W, half))
        col = np.broadcast_to(col[None, :, :], (rows, GRID_W, half))
        full = np.concatenate([row, col], -1).reshape(rows * GRID_W, HEAD_WIDTH)
        out.append(jnp.asarray(full[:length]))
    return out


def on_device(parts, groups, tokens, in_gain, query_weight, key_weight, value_matrix,
              query_gain, key_gain, out_weight, out_gain):
    sequence = tokens[0]
    row_count = sequence.shape[0]
    q_heads = QUERY_HEAD_COUNT // parts
    kv_heads = max(1, KEY_VALUE_HEADS // parts)
    per_group = QUERY_HEAD_COUNT // KEY_VALUE_HEADS
    cosine, sine = rotation(parts * row_count)
    rows, columns, out_head, own_tail = gather(
        sequence, query_weight, key_weight, value_matrix, out_weight, parts, groups // 2,
        q_heads * HEAD_WIDTH, kv_heads * HEAD_WIDTH, lambda sp: sp * q_heads // per_group)
    out_tail = lax.all_gather(own_tail, "dp", axis=0, tiled=True)
    q, k, v = project(rows, in_gain, columns, query_gain, key_gain, cosine, sine, q_heads, kv_heads, row_count)
    attended = attend(q, k, v, q_heads, kv_heads, row_count)
    returned = exchange(attended, parts)
    return output(returned, out_head, out_tail, out_gain)[None]


def solution(mesh):
    placed = (P("dp", "sp", None), P(), P("dp", None), P("dp", None), P("dp", None),
              P(), P(), P("dp", None), P())
    return jax.shard_map(
        functools.partial(on_device, mesh.shape["sp"], mesh.shape["dp"]),
        mesh=mesh, in_specs=placed, out_specs=P("dp", "sp", None), check_vma=False,
    )
```

```python
import functools

import jax
import jax.numpy as jnp
import numpy as np
from jax import lax
from jax.experimental import pallas as pl
from jax.experimental.pallas import tpu as pltpu
from jax.sharding import PartitionSpec as P

QUERY_HEAD_COUNT = 16
KEY_VALUE_HEADS = 4
HEAD_WIDTH = 128
GRID_W = 64
EPS = 1e-06
THETA = 10000.0
MESH = pl.DeviceIdType.MESH
ANY = pl.BlockSpec(memory_space=pl.ANY)


def remote(src, dst, send_sem, recv_sem, device):
    return pltpu.make_async_remote_copy(
        src_ref=src, dst_ref=dst, send_sem=send_sem, recv_sem=recv_sem,
        device_id=device, device_id_type=MESH,
    )


def gather_kernel(
    parts, chips, q_width, kv_width, first_kv_of,
    x_ref, wq_ref, wk_ref, wv_ref, wo_ref, rows_ref, cols_ref, head_ref, tail_ref,
    stage, x_send, x_recv, own_sem, stage_sem,
    up_send, up_recv, down_send, down_recv, pair_send, pair_recv,
):
    sp, dp = lax.axis_index("sp"), lax.axis_index("dp")
    z, core = dp // 2, dp % 2
    partner = z * 2 + (1 - core)
    row_count = x_ref.shape[0]
    depth = stage.shape[0]
    square = parts == 4

    first_kv = first_kv_of(sp)
    loads = [
        pltpu.make_async_copy(
            wq_ref.at[:, pl.ds(pl.multiple_of(sp * q_width, 128), q_width)],
            stage.at[:, pl.ds(0, q_width)], stage_sem.at[0]),
        pltpu.make_async_copy(
            wk_ref.at[:, pl.ds(pl.multiple_of(first_kv * HEAD_WIDTH, 128), kv_width)],
            stage.at[:, pl.ds(q_width, kv_width)], stage_sem.at[1]),
        pltpu.make_async_copy(
            wv_ref.at[:, pl.ds(pl.multiple_of(first_kv * HEAD_WIDTH, 128), kv_width)],
            stage.at[:, pl.ds(q_width + kv_width, kv_width)], stage_sem.at[2]),
    ]
    for load in loads:
        load.start()

    barrier = pltpu.get_barrier_semaphore()
    if square:
        x_side = (sp // 2) * 2 + (1 - sp % 2)
        y_side = (1 - sp // 2) * 2 + sp % 2
        corner = (1 - sp // 2) * 2 + (1 - sp % 2)
        greeted = [x_side, y_side]
    else:
        greeted = [lax.rem(sp + i, parts) for i in range(1, parts)]
    for peer in greeted:
        pl.semaphore_signal(barrier, inc=1, device_id={"sp": peer, "dp": dp}, device_id_type=MESH)
    pl.semaphore_signal(barrier, inc=1, device_id={"sp": sp, "dp": partner}, device_id_type=MESH)

    @pl.when(z < chips - 1)
    def _():
        pl.semaphore_signal(barrier, inc=1, device_id={"sp": sp, "dp": dp + 2}, device_id_type=MESH)

    @pl.when(z > 0)
    def _():
        pl.semaphore_signal(barrier, inc=1, device_id={"sp": sp, "dp": dp - 2}, device_id_type=MESH)

    in_chain = (z + chips - 1) // chips + (2 * chips - 2 - z) // chips
    pl.semaphore_wait(barrier, len(greeted) + 1 + in_chain)

    def token_rows(owner, half=None):
        if half is None:
            return rows_ref.at[pl.ds(owner * row_count, row_count)]
        return rows_ref.at[pl.ds(owner * row_count + half * (row_count // 2), row_count // 2)]

    token_sends = []
    if square:
        for half_x, half_y in ((0, 1), (1, 0)):
            for slot, half, peer in ((0, half_x, x_side), (1, half_y, y_side)):
                copy = remote(
                    x_ref.at[pl.ds(half * (row_count // 2), row_count // 2)],
                    token_rows(sp, half), x_send.at[slot * 2 + half],
                    x_recv.at[slot * 2 + half], {"sp": peer, "dp": dp})
                copy.start()
                token_sends.append(copy)
    else:
        for i, peer in enumerate(greeted):
            copy = remote(
                x_ref, token_rows(sp), x_send.at[i], x_recv.at[i], {"sp": peer, "dp": dp})
            copy.start()
            token_sends.append(copy)
    own_rows = pltpu.make_async_copy(x_ref, token_rows(sp), own_sem.at[0])
    own_rows.start()
    split = head_ref.shape[1]
    out_head = wo_ref.at[:, pl.ds(0, split)]
    own_tail = pltpu.make_async_copy(
        wo_ref.at[:, pl.ds(split, tail_ref.shape[1])], tail_ref, own_sem.at[2])
    own_tail.start()

    for load in loads:
        load.wait()

    gathered = (cols_ref, head_ref)
    sources = (stage, out_head)

    def block(t, owner_z, owner_core):
        return gathered[t].at[pl.ds((owner_z * 2 + owner_core) * depth, depth)]

    def to_up(t, src, k):
        return remote(src, block(t, z - k, core), up_send.at[t, k], up_recv.at[t, k + 1],
                      {"sp": sp, "dp": dp + 2})

    def to_down(t, src, k):
        return remote(src, block(t, z + k, core), down_send.at[t, k], down_recv.at[t, k + 1],
                      {"sp": sp, "dp": dp - 2})

    def to_pair(t, src, owner_z):
        return remote(src, block(t, owner_z, core), pair_send.at[t, owner_z],
                      pair_recv.at[t, owner_z], {"sp": sp, "dp": partner})

    own_copies = []
    for t in range(2):
        @pl.when(z < chips - 1)
        def _():
            to_up(t, sources[t], 0).start()

        @pl.when(z > 0)
        def _():
            to_down(t, sources[t], 0).start()

        to_pair(t, sources[t], z).start()
        own = pltpu.make_async_copy(sources[t], block(t, z, core), own_sem.at[(1, 3)[t]])
        own.start()
        own_copies.append(own)

    if square:
        got_x = remote(x_ref.at[pl.ds(0, row_count // 2)], token_rows(x_side, 0),
                       x_send.at[0], x_recv.at[0], {"sp": x_side, "dp": dp})
        got_y = remote(x_ref.at[pl.ds(0, row_count // 2)], token_rows(y_side, 1),
                       x_send.at[3], x_recv.at[3], {"sp": y_side, "dp": dp})

    def relay_columns(t, k):
        @pl.when(z >= k)
        def _():
            source = block(t, z - k, core)
            remote(source, source, up_send.at[t, k], up_recv.at[t, k],
                   {"sp": sp, "dp": partner}).wait_recv()
            if k < chips - 1:
                @pl.when(z < chips - 1)
                def _():
                    to_up(t, source, k).start()
            to_pair(t, source, z - k).start()

        @pl.when(z + k <= chips - 1)
        def _():
            source = block(t, z + k, core)
            remote(source, source, down_send.at[t, k], down_recv.at[t, k],
                   {"sp": sp, "dp": partner}).wait_recv()
            if k < chips - 1:
                @pl.when(z > 0)
                def _():
                    to_down(t, source, k).start()
            to_pair(t, source, z + k).start()

    if chips > 1:
        relay_columns(0, 1)
    if square:
        got_x.wait_recv()
        relay_x = remote(token_rows(x_side, 0), token_rows(x_side, 0),
                         x_send.at[4], x_recv.at[4], {"sp": y_side, "dp": dp})
        relay_x.start()
        got_y.wait_recv()
        relay_y = remote(token_rows(y_side, 1), token_rows(y_side, 1),
                         x_send.at[5], x_recv.at[5], {"sp": x_side, "dp": dp})
        relay_y.start()
        token_sends += [relay_x, relay_y]
    for k in range(1, chips):
        if k > 1:
            relay_columns(0, k)
        relay_columns(1, k)

    for t in range(2):
        for owner_z in range(chips):
            source = block(t, owner_z, 1 - core)
            remote(source, source, pair_send.at[t, owner_z], pair_recv.at[t, owner_z],
                   {"sp": sp, "dp": partner}).wait_recv()
    if square:
        for owner, half, slot in (
            (x_side, 1, 1), (y_side, 0, 2), (corner, 0, 4), (corner, 1, 5)
        ):
            target = token_rows(owner, half)
            remote(target, target, x_send.at[slot], x_recv.at[slot],
                   {"sp": x_side, "dp": dp}).wait_recv()
    else:
        for i in range(parts - 1):
            target = token_rows(lax.rem(sp + parts - 1 - i, parts))
            remote(target, target, x_send.at[i], x_recv.at[i],
                   {"sp": greeted[0], "dp": dp}).wait_recv()
    for copy in token_sends:
        copy.wait_send()
    for t in range(2):
        for owner_z in range(chips):
            to_pair(t, sources[t], owner_z).wait_send()
        for k in range(chips - 1):
            @pl.when(jnp.logical_and(z < chips - 1, z >= k))
            def _():
                to_up(t, sources[t], k).wait_send()

            @pl.when(jnp.logical_and(z > 0, z + k <= chips - 1))
            def _():
                to_down(t, sources[t], k).wait_send()
    own_rows.wait()
    own_tail.wait()
    for own in own_copies:
        own.wait()


def gather(sequence, query_weight, key_weight, value_matrix, out_weight, parts, chips, q_width, kv_width, first_kv_of):
    depth, width = query_weight.shape[0], q_width + 2 * kv_width
    row_count, features = sequence.shape
    dma = pltpu.SemaphoreType.DMA
    chain = dma((2, chips + 1))
    split = out_weight.shape[1] * 5 // 8
    return pl.pallas_call(
        functools.partial(gather_kernel, parts, chips, q_width, kv_width, first_kv_of),
        out_shape=(
            jax.ShapeDtypeStruct((parts * row_count, features), jnp.bfloat16),
            jax.ShapeDtypeStruct((chips * 2 * depth, width), jnp.bfloat16),
            jax.ShapeDtypeStruct((chips * 2 * depth, split), jnp.bfloat16),
            jax.ShapeDtypeStruct((depth, out_weight.shape[1] - split), jnp.bfloat16),
        ),
        in_specs=[pl.BlockSpec(memory_space=pltpu.VMEM), ANY, ANY, ANY,
                  pl.BlockSpec(memory_space=pltpu.VMEM)],
        out_specs=(ANY, ANY, ANY, ANY),
        scratch_shapes=[
            pltpu.VMEM((depth, width), jnp.bfloat16),
            dma((max(6, parts),)), dma((max(6, parts),)), dma((4,)), dma((3,)),
            chain, chain, chain, chain, chain, chain,
        ],
        compiler_params=pltpu.CompilerParams(collective_id=0, has_side_effects=True),
        cost_estimate=pl.CostEstimate(flops=40_000_000_000, bytes_accessed=100_000_000, transcendentals=0),
        name="gather_rows_columns",
    )(sequence, query_weight, key_weight, value_matrix, out_weight)


def exchange_kernel(parts, a_ref, o_ref, send, recv, own_sem):
    sp, dp = lax.axis_index("sp"), lax.axis_index("dp")
    row_count = o_ref.shape[1]
    barrier = pltpu.get_barrier_semaphore()
    peers = [lax.rem(sp + i, parts) for i in range(1, parts)]
    for peer in peers:
        pl.semaphore_signal(barrier, inc=1, device_id={"sp": peer, "dp": dp}, device_id_type=MESH)
    pl.semaphore_wait(barrier, parts - 1)
    copies = []
    for i, peer in enumerate(peers):
        copy = remote(a_ref.at[pl.ds(peer * row_count, row_count)], o_ref.at[sp],
                      send.at[i], recv.at[i], {"sp": peer, "dp": dp})
        copy.start()
        copies.append(copy)
    own = pltpu.make_async_copy(a_ref.at[pl.ds(sp * row_count, row_count)], o_ref.at[sp], own_sem)
    own.start()
    for i in range(parts - 1):
        target = o_ref.at[lax.rem(sp + parts - 1 - i, parts)]
        remote(target, target, send.at[i], recv.at[i], {"sp": peers[0], "dp": dp}).wait_recv()
    for copy in copies:
        copy.wait_send()
    own.wait()


def exchange(attended, parts):
    length, width = attended.shape
    row_count = length // parts
    dma = pltpu.SemaphoreType.DMA
    return pl.pallas_call(
        functools.partial(exchange_kernel, parts),
        out_shape=jax.ShapeDtypeStruct((parts, row_count, width), jnp.bfloat16),
        in_specs=[pl.BlockSpec(memory_space=pltpu.VMEM)],
        out_specs=ANY,
        scratch_shapes=[dma((parts,)), dma((parts,)), dma],
        compiler_params=pltpu.CompilerParams(collective_id=1, has_side_effects=True),
        cost_estimate=pl.CostEstimate(flops=10_000_000_000, bytes_accessed=20_000_000, transcendentals=0),
        name="exchange_heads",
    )(attended)


def project_kernel(q_heads, kv_heads, x_ref, g_ref, w_ref, qg_ref, kg_ref, cos_ref, sin_ref,
                   q_ref, k_ref, v_ref):
    x = x_ref[...].astype(jnp.float32)
    scale = lax.rsqrt(jnp.mean(x * x, axis=-1, keepdims=True) + EPS)
    normed = (x * scale * g_ref[...]).astype(jnp.bfloat16)
    mixed = jnp.dot(normed, w_ref[...], preferred_element_type=jnp.float32)
    cosine, sine = cos_ref[...], sin_ref[...]
    lane = lax.broadcasted_iota(jnp.int32, cosine.shape, 1)
    first = lane % (HEAD_WIDTH // 2) < HEAD_WIDTH // 4

    def finish(head, gain):
        head = head * lax.rsqrt(jnp.mean(head * head, axis=-1, keepdims=True) + EPS) * gain
        other = jnp.where(first, pltpu.roll(head, HEAD_WIDTH - HEAD_WIDTH // 4, 1),
                          pltpu.roll(head, HEAD_WIDTH // 4, 1))
        return (head * cosine + other * sine).astype(jnp.bfloat16)

    for h in range(q_heads):
        span = slice(h * HEAD_WIDTH, (h + 1) * HEAD_WIDTH)
        q_ref[:, span] = finish(mixed[:, span], qg_ref[...])
    for h in range(kv_heads):
        span = slice(h * HEAD_WIDTH, (h + 1) * HEAD_WIDTH)
        start = (q_heads + h) * HEAD_WIDTH
        k_ref[:, span] = finish(mixed[:, start:start + HEAD_WIDTH], kg_ref[...])
    v_ref[...] = mixed[:, (q_heads + kv_heads) * HEAD_WIDTH:].astype(jnp.bfloat16)


def project(rows, in_gain, columns, query_gain, key_gain, cosine, sine, q_heads, kv_heads, row_block):
    length, features = rows.shape
    width = columns.shape[1]
    q_width, kv_width = q_heads * HEAD_WIDTH, kv_heads * HEAD_WIDTH
    whole = lambda shape: pl.BlockSpec(shape, lambda i: (0, 0))
    part = lambda size: pl.BlockSpec((row_block, size), lambda i: (i, 0))
    return pl.pallas_call(
        functools.partial(project_kernel, q_heads, kv_heads),
        grid=(length // row_block,),
        out_shape=tuple(jax.ShapeDtypeStruct((length, n), jnp.bfloat16) for n in (q_width, kv_width, kv_width)),
        in_specs=[part(features), whole((1, features)), whole((features, width)),
                  whole((1, HEAD_WIDTH)), whole((1, HEAD_WIDTH)), part(HEAD_WIDTH), part(HEAD_WIDTH)],
        out_specs=(part(q_width), part(kv_width), part(kv_width)),
        cost_estimate=pl.CostEstimate(flops=2 * length * features * width, bytes_accessed=9_000_000, transcendentals=0),
        name="project_heads",
    )(rows, in_gain[None], columns, query_gain[None], key_gain[None], cosine, sine)


def attend_kernel(group, q_ref, k_ref, v_ref, o_ref):
    factor = HEAD_WIDTH ** (-0.5) * float(np.log2(np.e))
    for h in range(q_ref.shape[1] // HEAD_WIDTH):
        span = slice(h * HEAD_WIDTH, (h + 1) * HEAD_WIDTH)
        shared = slice(h // group * HEAD_WIDTH, (h // group + 1) * HEAD_WIDTH)
        scores = lax.dot_general(q_ref[:, span], k_ref[:, shared], (((1,), (1,)), ((), ())),
                                 preferred_element_type=jnp.float32)
        top = jnp.max(scores, axis=-1, keepdims=True)
        raised = jnp.exp2((scores - top) * factor)
        weights = (raised * (1.0 / jnp.sum(raised, axis=-1, keepdims=True))).astype(jnp.bfloat16)
        o_ref[:, span] = jnp.dot(
            weights, v_ref[:, shared], preferred_element_type=jnp.float32).astype(jnp.bfloat16)


def attend(q, k, v, q_heads, kv_heads, row_block):
    length = q.shape[0]
    block = pl.BlockSpec((row_block, q.shape[1]), lambda i: (i, 0))
    keys = pl.BlockSpec(k.shape, lambda i: (0, 0))
    return pl.pallas_call(
        functools.partial(attend_kernel, q_heads // kv_heads),
        grid=(length // row_block,),
        out_shape=jax.ShapeDtypeStruct(q.shape, jnp.bfloat16),
        in_specs=[block, keys, keys],
        out_specs=block,
        cost_estimate=pl.CostEstimate(flops=4 * length * length * q_heads * HEAD_WIDTH,
                                      bytes_accessed=3_000_000, transcendentals=length * length * q_heads),
        name="attend_heads",
    )(q, k, v)


def output_kernel(a_ref, head_ref, tail_ref, g_ref, o_ref, total):
    step = pl.program_id(0)
    split = head_ref.shape[1]

    @pl.when(step == 0)
    def _():
        total[...] = jnp.zeros_like(total)

    total[:, :split] += jnp.dot(a_ref[0], head_ref[...], preferred_element_type=jnp.float32)
    total[:, split:] += jnp.dot(a_ref[0], tail_ref[...], preferred_element_type=jnp.float32)

    @pl.when(step == pl.num_programs(0) - 1)
    def _():
        x = total[...]
        scale = lax.rsqrt(jnp.mean(x * x, axis=-1, keepdims=True) + EPS)
        o_ref[...] = (x * scale * g_ref[...]).astype(jnp.bfloat16)


def output(returned, out_head, out_tail, out_gain):
    parts, row_count, width = returned.shape
    features = out_gain.shape[0]
    split = out_head.shape[1]
    return pl.pallas_call(
        output_kernel,
        grid=(parts,),
        out_shape=jax.ShapeDtypeStruct((row_count, features), jnp.bfloat16),
        in_specs=[pl.BlockSpec((1, row_count, width), lambda s: (s, 0, 0)),
                  pl.BlockSpec((width, split), lambda s: (s, 0)),
                  pl.BlockSpec((width, features - split), lambda s: (s, 0)),
                  pl.BlockSpec((1, features), lambda s: (0, 0))],
        out_specs=pl.BlockSpec((row_count, features), lambda s: (0, 0)),
        scratch_shapes=[pltpu.VMEM((row_count, features), jnp.float32)],
        cost_estimate=pl.CostEstimate(flops=2 * row_count * features * width * parts,
                                      bytes_accessed=10_000_000, transcendentals=0),
        name="output_rows",
    )(returned, out_head, out_tail, out_gain[None])


def rotation(length):
    quarter = HEAD_WIDTH // 4
    inverse_freq = (THETA ** (-np.arange(quarter, dtype=np.float32) / quarter)).astype(np.float32)

    def table(count):
        angle = (np.arange(count, dtype=np.float32)[:, None] * inverse_freq[None, :]).astype(np.float64)
        cosine, sine = np.cos(angle), np.sin(angle)
        return (np.concatenate([cosine, cosine], 1).astype(np.float32),
                np.concatenate([-sine, sine], 1).astype(np.float32))

    rows = -(-length // GRID_W)
    row_tables, col_tables = table(rows), table(GRID_W)
    half = HEAD_WIDTH // 2
    out = []
    for row, col in zip(row_tables, col_tables):
        row = np.broadcast_to(row[:, None, :], (rows, GRID_W, half))
        col = np.broadcast_to(col[None, :, :], (rows, GRID_W, half))
        full = np.concatenate([row, col], -1).reshape(rows * GRID_W, HEAD_WIDTH)
        out.append(jnp.asarray(full[:length]))
    return out


def on_device(parts, groups, tokens, in_gain, query_weight, key_weight, value_matrix,
              query_gain, key_gain, out_weight, out_gain):
    sequence = tokens[0]
    row_count = sequence.shape[0]
    q_heads = QUERY_HEAD_COUNT // parts
    kv_heads = max(1, KEY_VALUE_HEADS // parts)
    per_group = QUERY_HEAD_COUNT // KEY_VALUE_HEADS
    cosine, sine = rotation(parts * row_count)
    rows, columns, out_head, own_tail = gather(
        sequence, query_weight, key_weight, value_matrix, out_weight, parts, groups // 2,
        q_heads * HEAD_WIDTH, kv_heads * HEAD_WIDTH, lambda sp: sp * q_heads // per_group)
    out_tail = lax.all_gather(own_tail, "dp", axis=0, tiled=True)
    q, k, v = project(rows, in_gain, columns, query_gain, key_gain, cosine, sine, q_heads, kv_heads, row_count)
    attended = attend(q, k, v, q_heads, kv_heads, row_count)
    returned = exchange(attended, parts)
    return output(returned, out_head, out_tail, out_gain)[None]


def solution(mesh):
    placed = (P("dp", "sp", None), P(), P("dp", None), P("dp", None), P("dp", None),
              P(), P(), P("dp", None), P())
    return jax.shard_map(
        functools.partial(on_device, mesh.shape["sp"], mesh.shape["dp"]),
        mesh=mesh, in_specs=placed, out_specs=P("dp", "sp", None), check_vma=False,
    )
```
